32 devices in a mesh: grp: 2 (over x), tp: 16 (over z, y, core).
Axes of the slice: x: 2, y: 2, z: 4, core: 2. Of those that a mesh axis runs over, the one named last changes fastest.
Arguments:
- tokens: bfloat16 [160, 2048], P('grp', 'tp'), parts along dimension 0, may hold values from -6 to 6
- lengths: int32 [160], P('grp'), parts along dimension 0, may hold values from 1 to 4096, 81920 in all
- cell_memory: float32 [2, 160, 2048, 256], P(None, 'grp', 'tp'), parts along dimension 1, may hold values from -0.6 to 0.6
- key_sums: float32 [2, 160, 2048], P(None, 'grp', 'tp'), parts along dimension 1, may hold values from -3 to 3
- stabilizer: float32 [2, 160, 8], P(None, 'grp'), parts along dimension 1, may hold values from -3 to 1
- norm_gain: bfloat16 [2, 2048], replicated, may hold values from 0.099609375 to 1.8984375
- query_weight: bfloat16 [2, 2048, 2048], P(None, None, 'tp'), may hold values from -0.125 to 0.125
- key_weight: bfloat16 [2, 2048, 2048], P(None, None, 'tp'), may hold values from -0.125 to 0.125
- value_weight: bfloat16 [2, 2048, 2048], P(None, None, 'tp'), may hold values from -0.125 to 0.125
- outgate_weight: bfloat16 [2, 2048, 2048], P(None, None, 'tp'), may hold values from -0.125 to 0.125
- ingate_weight: bfloat16 [2, 2048, 8], replicated, may hold values from -0.125 to 0.125
- forget_weight: bfloat16 [2, 2048, 8], replicated, may hold values from -0.125 to 0.125
- ingate_bias: float32 [2, 8], replicated, may hold values from -3 to 3
- forget_bias: float32 [2, 8], replicated, may hold values from -1 to 4
- forget_slope: float32 [2, 8], replicated, may hold values from -3 to 3
- head_gain: bfloat16 [2, 2048], P(None, 'tp'), may hold values from 0.099609375 to 1.8984375
- output_weight: bfloat16 [2, 2048, 2048], P(None, None, 'tp'), may hold values from -0.125 to 0.125
Outputs:
- new_tokens: bfloat16 [160, 2048], P('grp', 'tp'), parts along dimension 0
- new_memory: float32 [2, 160, 2048, 256], P(None, 'grp', 'tp'), parts along dimension 1
- new_key_sums: float32 [2, 160, 2048], P(None, 'grp', 'tp'), parts along dimension 1
- new_stabilizer: float32 [2, 160, 8], P(None, 'grp'), parts along dimension 1
The draws below stay inside these ranges and needn't reach their ends.
There are 2 independent parts, one for each index of `grp`. The reference program is written for one: setup_inputs(seed, part) draws one part's arguments, and reference() takes and returns one part's arrays. A program takes and returns all parts, laid end to end along the dimension named above; an argument that names none is the same for every part. Nothing has to cross between parts.
Inputs may be any that keep to these rules, and one draw needn't show every extreme that they name: Each part's 80 lengths sum to 81920, and the largest is exactly 4096.
All inputs are finite; a program needn't handle non-finite values.
Results may differ from the reference program's by a relative error of at most 0.018.
Values may be sent and summed in bfloat16 or wider, within the bound.
A program may use at most 128 MiB of HBM per device.

```python
import math
import jax
import jax.numpy as jnp
import numpy as np
from jax import lax

HEADS = 8
HEAD = 256
D = 2048
BATCH = 80
BLOCKS = 2
MEANLEN = 1024
MAXLEN = 4096


def shard_levels(stream_key, dims, shards, low, high):
    gain, own = 1.0, jax.random.fold_in(stream_key, 6)
    for dim, parts in shards:
        heights = jnp.exp(jax.random.uniform(jax.random.fold_in(own, dim), (parts,), jnp.float32, low / len(shards), high / len(shards)))
        gain = gain * jnp.repeat(heights, dims[dim] // parts).reshape([-1 if axis == dim else 1 for axis in range(len(dims))])
    return gain


def split_up(count, total, most, skew):
    portions = [(1 << 20) // math.isqrt(standing ** skew) + 1 for standing in range(2, count + 1)]
    rest, given = total - most - (count - 1), [1] * (count - 1)
    while rest > 0:
        movable = [i for i in range(count - 1) if given[i] < most]
        pool, budget = sum([portions[i] for i in movable]), rest
        for i in movable:
            addition = min(most - given[i], max(1, budget * portions[i] // pool), rest)
            given[i] = given[i] + addition
            rest = rest - addition
    return np.array([most] + given)


def uneven_parts(own_key, amount, total, reach, slope):
    if amount == 2:
        one = jax.random.randint(own_key, (), max(1, total - reach), min(reach, total - 1) + 1)
        return jnp.stack([one, total - one])
    sizes = jnp.asarray(split_up(amount, total, reach, slope), jnp.int32)
    pairs = (amount - 1) // 2
    donor, taker = sizes[1:1 + 2 * pairs:2], sizes[2:2 + 2 * pairs:2]
    margin = jnp.minimum(donor - 1, reach - taker)
    moved = jax.random.randint(jax.random.fold_in(own_key, 1), (pairs,), 0, 1 << 20) % (margin + 1)
    sizes = sizes.at[1:1 + 2 * pairs:2].set(donor - moved).at[2:2 + 2 * pairs:2].set(taker + moved)
    return sizes[jax.random.permutation(jax.random.fold_in(own_key, 2), amount)]


def scatter_about(stream_key, dims, width, reach, cuts=(), held_as=jnp.bfloat16):
    result = width * jax.random.normal(stream_key, dims, jnp.float32)
    if cuts:
        result = result * shard_levels(stream_key, dims, cuts, -0.22, 0.18)
    return jnp.clip(result, -reach, reach).astype(held_as)


def setup_inputs(seed: int = 0, part: int = 0) -> dict:
    streams_of = jax.random.split(jax.random.key(seed), 18)
    own_keys = jax.random.split(jax.random.fold_in(streams_of[17], part), 18)
    tokens = scatter_about(own_keys[0], (BATCH, D), 1.0, 6.0, ((1, 16),))
    lengths = uneven_parts(own_keys[1], BATCH, BATCH * MEANLEN, MAXLEN, 2).astype(jnp.int32)
    cell_memory = scatter_about(own_keys[2], (BLOCKS, BATCH, D, HEAD), 0.1, 0.6, ((2, 16),), jnp.float32)
    key_sums = scatter_about(own_keys[3], (BLOCKS, BATCH, D), 0.5, 3.0, ((2, 16),), jnp.float32)
    stabilizer = jnp.clip(jax.random.uniform(own_keys[4], (BLOCKS, BATCH, HEADS), jnp.float32, -3.0, 1.0), -3.0, 1.0)
    norm_gain = jnp.clip(1.0 + 0.18 * jax.random.normal(streams_of[5], (BLOCKS, D), jnp.float32), 0.099609375, 1.8984375).astype(jnp.bfloat16)
    query_weight = scatter_about(streams_of[6], (BLOCKS, D, D), D ** -0.5, 0.125, ((2, 16),))
    key_weight = scatter_about(streams_of[7], (BLOCKS, D, D), D ** -0.5, 0.125, ((2, 16),))
    value_weight = scatter_about(streams_of[8], (BLOCKS, D, D), D ** -0.5, 0.125, ((2, 16),))
    outgate_weight = scatter_about(streams_of[9], (BLOCKS, D, D), D ** -0.5, 0.125, ((2, 16),))
    ingate_weight = scatter_about(streams_of[10], (BLOCKS, D, HEADS), D ** -0.5, 0.125)
    forget_weight = scatter_about(streams_of[11], (BLOCKS, D, HEADS), D ** -0.5, 0.125)
    ingate_bias = scatter_about(streams_of[12], (BLOCKS, HEADS), 1.0, 3.0, (), jnp.float32)
    forget_bias = jnp.clip(jax.random.uniform(streams_of[13], (BLOCKS, HEADS), jnp.float32, -1.0, 4.0), -1.0, 4.0)
    forget_slope = jnp.clip(jax.random.uniform(streams_of[14], (BLOCKS, HEADS), jnp.float32, -3.0, 3.0), -3.0, 3.0)
    head_gain = jnp.clip(1.0 + 0.18 * jax.random.normal(streams_of[15], (BLOCKS, D), jnp.float32), 0.099609375, 1.8984375).astype(jnp.bfloat16)
    output_weight = scatter_about(streams_of[16], (BLOCKS, D, D), D ** -0.5, 0.125, ((2, 16),))
    return dict(tokens=tokens, lengths=lengths, cell_memory=cell_memory, key_sums=key_sums, stabilizer=stabilizer, norm_gain=norm_gain, query_weight=query_weight, key_weight=key_weight, value_weight=value_weight, outgate_weight=outgate_weight, ingate_weight=ingate_weight, forget_weight=forget_weight, ingate_bias=ingate_bias, forget_bias=forget_bias, forget_slope=forget_slope, head_gain=head_gain, output_weight=output_weight)


EPS = 1e-05

def one_block(tokens, position, memory, key_sums, stabilizer, norm_gain, query_weight, key_weight, value_weight, outgate_weight, ingate_weight, forget_weight, ingate_bias, forget_bias, forget_slope, head_gain, output_weight):
    batch_rows = tokens.shape[0]
    model_width = tokens.shape[1]
    head_count = stabilizer.shape[1]
    head_size = model_width // head_count
    tok_float = tokens.astype(jnp.float32)
    normed = (tok_float * lax.rsqrt(lax.optimization_barrier(jnp.mean(tok_float * tok_float, axis=-1, keepdims=True)) + EPS) * norm_gain.astype(jnp.float32)).astype(jnp.bfloat16)
    queries = jnp.dot(normed, query_weight, preferred_element_type=jnp.float32).astype(jnp.bfloat16)
    key_rows = (jnp.dot(normed, key_weight, preferred_element_type=jnp.float32) * head_size ** (-0.5)).astype(jnp.bfloat16)
    values = jnp.dot(normed, value_weight, preferred_element_type=jnp.float32).astype(jnp.bfloat16)
    outgate = jnp.dot(normed, outgate_weight, preferred_element_type=jnp.float32).astype(jnp.bfloat16)
    ingate = jnp.dot(normed, ingate_weight, preferred_element_type=jnp.float32) + ingate_bias
    forget = jax.nn.log_sigmoid(jnp.dot(normed, forget_weight, preferred_element_type=jnp.float32) + forget_bias + forget_slope * position[:, None])
    stab_new = jnp.maximum(forget + stabilizer, ingate)
    decays = jnp.exp(forget + stabilizer - stab_new)
    in_weight = jnp.exp(ingate - stab_new)
    query_heads = queries.astype(jnp.float32).reshape(batch_rows, head_count, head_size)
    key_heads = key_rows.astype(jnp.float32).reshape(batch_rows, head_count, head_size)
    value_heads = values.astype(jnp.float32).reshape(batch_rows, head_count, head_size)
    old_memory = memory.reshape(batch_rows, head_count, head_size, head_size)
    mem_new = decays[:, :, None, None] * old_memory + in_weight[:, :, None, None] * value_heads[:, :, :, None] * key_heads[:, :, None, :]
    sums_new = decays[:, :, None] * key_sums.reshape(batch_rows, head_count, head_size) + in_weight[:, :, None] * key_heads
    numerator = jnp.einsum('bhvk,bhk->bhv', mem_new, query_heads, precision=lax.Precision.HIGHEST)
    denominator = jnp.maximum(jnp.abs(lax.optimization_barrier(jnp.sum(sums_new * query_heads, axis=-1))), 1.0)
    hidden = numerator / denominator[:, :, None]
    gated_out = (hidden.reshape(batch_rows, model_width) * head_gain.astype(jnp.float32) * jax.nn.sigmoid(outgate.astype(jnp.float32))).astype(jnp.bfloat16)
    new_tokens = (tok_float + jnp.dot(gated_out, output_weight, preferred_element_type=jnp.float32)).astype(jnp.bfloat16)
    return (new_tokens, mem_new.reshape(batch_rows, model_width, head_size), sums_new.reshape(batch_rows, model_width), stab_new)

def reference(tokens, lengths, cell_memory, key_sums, stabilizer, norm_gain, query_weight, key_weight, value_weight, outgate_weight, ingate_weight, forget_weight, ingate_bias, forget_bias, forget_slope, head_gain, output_weight):
    position = lengths.astype(jnp.float32) / MAXLEN
    current = tokens
    memories, sums_list, stabs = ([], [], [])
    for block_id in range(BLOCKS):
        current, mem_new, sums_new, stab_new = one_block(current, position, cell_memory[block_id], key_sums[block_id], stabilizer[block_id], norm_gain[block_id], query_weight[block_id], key_weight[block_id], value_weight[block_id], outgate_weight[block_id], ingate_weight[block_id], forget_weight[block_id], ingate_bias[block_id], forget_bias[block_id], forget_slope[block_id], head_gain[block_id], output_weight[block_id])
        memories.append(mem_new)
        sums_list.append(sums_new)
        stabs.append(stab_new)
    return (current, jnp.stack(memories), jnp.stack(sums_list), jnp.stack(stabs))
```

```python
import functools

import jax
import jax.numpy as jnp
from jax import lax
from jax.experimental import pallas as pl
from jax.experimental.pallas import tpu as pltpu
from jax.sharding import PartitionSpec as P

HEADS = 8
HEAD = 256
MAXLEN = 4096
EPS = 1e-05
MESH = pl.DeviceIdType.MESH
F32 = jnp.float32
BF16 = jnp.bfloat16
GROUP = 8


def parts_of(batch):
    first = (batch + 31) // 32 * 16
    return ((0, first), (first, batch - first))


def kernel(
    n,
    tokens,
    lengths,
    cell_memory,
    key_sums,
    stabilizer,
    norm_gain,
    query_weight,
    key_weight,
    value_weight,
    outgate_weight,
    ingate_weight,
    forget_weight,
    ingate_bias,
    forget_bias,
    forget_slope,
    head_gain,
    output_weight,
    new_tokens,
    mem,
    new_sums,
    new_stab,
    lengths_in,
    stabilizer_in,
    norm_gain_in,
    ingate_bias_in,
    forget_bias_in,
    forget_slope_in,
    head_gain_in,
    wbig,
    wout,
    wgi,
    wgate,
    small_sem,
    gath,
    sums,
    vt_ref,
    decay_ref,
    kk_ref,
    local_sem,
    mem_sem,
    gsend,
    gfwd,
    grecv,
    wsend,
    wrecv,
    ssend,
    srecv,
):
    blocks, batch, rows, head = mem.shape
    heads = stabilizer.shape[1]
    width = output_weight.shape[1]
    split = n // heads
    chips = n // 2
    me = lax.axis_index("tp")
    chip = me // 2
    core = lax.rem(me, 2)
    sibling = me + 1 - 2 * core
    own_head = me // split
    lanes = pl.multiple_of
    parts = parts_of(batch)

    half, quarter = chips // 2, chips // 4
    flip = chip // half
    seat = chip + flip * (chips - 1 - 2 * chip)

    def unflip(d):
        return d + flip * (chips - 1 - 2 * d)

    far_chips = [unflip(chips - 1 - i) for i in range(half)]
    near_chips = [unflip(lax.rem(seat + i, half)) for i in range(1, half)]
    far_group = 2 - seat // quarter
    targets = [(c, far_group) for c in far_chips] + [(c, 0) for c in near_chips]
    groups = (
        near_chips,
        [unflip(half + i) for i in range(quarter)],
        [unflip(half + quarter + i) for i in range(quarter)],
    )

    own_copy = pltpu.make_async_copy(tokens, gath.at[0, me], local_sem.at[0, 3])
    own_copy.start()
    sums_copy = pltpu.make_async_copy(key_sums, sums.at[core], local_sem.at[1, 3])
    small = [
        pltpu.make_async_copy(a, b, small_sem.at[i])
        for i, (a, b) in enumerate(
            (
                (lengths, lengths_in),
                (stabilizer, stabilizer_in),
                (norm_gain, norm_gain_in),
                (ingate_bias, ingate_bias_in),
                (forget_bias, forget_bias_in),
                (forget_slope, forget_slope_in),
                (head_gain, head_gain_in),
            )
        )
    ]
    own_query = pl.ds(lanes(core * rows, rows), rows)
    own_key = pl.ds(lanes(head + core * rows, rows), rows)
    places = (own_query, own_key, pl.ds(2 * head, rows), pl.ds(2 * head + rows, rows))

    def load(l):
        for i, w in enumerate((query_weight, key_weight, value_weight, outgate_weight)):
            pltpu.make_async_copy(w.at[l], wbig.at[l, :, places[i]], local_sem.at[l, 0]).start()
        pltpu.make_async_copy(ingate_weight.at[l], wgi.at[l, 0], local_sem.at[l, 1]).start()
        pltpu.make_async_copy(forget_weight.at[l], wgi.at[l, 1], local_sem.at[l, 1]).start()
        if l == 0:
            for c in small:
                c.start()
            sums_copy.start()
        own = wout.at[l, :, pl.ds(lanes(core * rows, rows), rows)]
        pltpu.make_async_copy(output_weight.at[l], own, local_sem.at[l, 2]).start()
        pltpu.make_async_copy(cell_memory.at[l], mem.at[l], mem_sem.at[l]).start()

    def loaded(ref, sem):
        pltpu.make_async_copy(ref, ref, sem).wait()

    load(0)

    barrier = pltpu.get_barrier_semaphore()
    pl.semaphore_signal(barrier, inc=1, device_id={"tp": sibling}, device_id_type=MESH)

    @pl.when(core == 1)
    def _():
        for c, _ in targets:
            for other in range(2):
                pl.semaphore_signal(
                    barrier, inc=1, device_id={"tp": c * 2 + other}, device_id_type=MESH
                )

    pl.semaphore_wait(barrier, chips)

    def remote(ref, send, recv, dest):
        return pltpu.make_async_remote_copy(
            src_ref=ref,
            dst_ref=ref,
            send_sem=send,
            recv_sem=recv,
            device_id={"tp": dest},
            device_id_type=MESH,
        )

    def block_copy(g, p, slot, group, send, dest):
        return remote(gath.at[g, slot, pl.ds(*parts[p])], send, grecv.at[g, p, group], dest)

    def pair_copy(g, p, c, group, send, dest):
        ref = gath.at[g, pl.ds(2 * c, 2), pl.ds(*parts[p])]
        return remote(ref, send, grecv.at[g, p, group], dest)

    def arrived(g, p, group, count):
        ref = gath.at[g, pl.ds(0, count), pl.ds(*parts[p])]
        remote(ref, gsend.at[g], grecv.at[g, p, group], sibling).wait_recv()

    def flushed(ref, sem):
        remote(ref, sem, wrecv.at[0, 0], sibling).wait_send()

    def send_own(g, p):
        for c, group in targets:
            block_copy(g, p, me, group, gsend.at[g], c * 2 + 1).start()

    def gathered(l, k):
        g = 2 * l
        if k < 0:
            for p in range(len(parts)):
                if l == 0:
                    arrived(g, p, 3, 1)
                else:

                    @pl.when(core == 0)
                    def _():
                        arrived(g, p, 3, 2)

            return [chip]
        for p in range(len(parts)):
            arrived(g, p, k, 2 * len(groups[k]))

            @pl.when(core == 1)
            def _():
                for c in groups[k]:
                    pair_copy(g, p, c, k, gfwd.at[l], sibling).start()

        return groups[k]

    own_copy.wait()
    for p in range(len(parts)):
        block_copy(0, p, me, 3, gsend.at[0], sibling).start()
        send_own(0, p)
    sums_copy.wait()
    sums_send = remote(sums.at[core], ssend, srecv, sibling)
    sums_send.start()

    def push_weights(l):
        loaded(wbig.at[l, :, pl.ds(0, 4 * rows)], local_sem.at[l, 0])
        for place in (own_query, own_key):
            remote(wbig.at[l, :, place], wsend.at[l, 0], wrecv.at[l, 0], sibling).start()
        loaded(wout.at[l, :, pl.ds(0, rows)], local_sem.at[l, 2])

        @pl.when(core == 0)
        def _():
            ref = wout.at[l, :, pl.ds(0, rows)]
            remote(ref, wsend.at[l, 1], wrecv.at[l, 1], sibling).start()

    push_weights(0)
    for l in range(1, blocks):
        load(l)
    for c in small:
        c.wait()
    eye = lax.broadcasted_iota(jnp.int32, (batch, batch), 0) == lax.broadcasted_iota(
        jnp.int32, (batch, batch), 1
    )
    position = jnp.sum(
        jnp.where(eye, lengths_in[...].astype(F32) / MAXLEN, 0.0), axis=1, keepdims=True
    )
    lane = lax.broadcasted_iota(jnp.int32, (rows, rows), 1)
    head_mask = lax.broadcasted_iota(jnp.int32, (batch, heads), 1) == own_head

    def project(l):
        old_stab = stabilizer_in[l].T
        bias = forget_bias_in[l : l + 1, :] + forget_slope_in[l : l + 1, :] * position

        def step(c, total):
            at = pl.ds(lanes(c * 2 * rows, 2 * rows), 2 * rows)
            x = jnp.concatenate((gath[2 * l, 2 * c], gath[2 * l, 2 * c + 1]), axis=1).astype(F32)
            gain = norm_gain_in[:, at].astype(F32)[l : l + 1]
            scaled = (x * gain).astype(BF16)
            part = jnp.dot(scaled, wbig[l, at, :], preferred_element_type=F32)
            gpart = lax.dot_general(
                scaled, wgate[l, :, at], (((1,), (1,)), ((), ())), preferred_element_type=F32
            )
            square = x * x
            if total is None:
                return part, gpart, square
            return total[0] + part, total[1] + gpart, total[2] + square

        total = None
        for k in range(-1, len(groups)):
            for c in gathered(l, k):
                total = step(c, total)
        proj, gates, square = total
        scale = lax.rsqrt(jnp.sum(square, axis=1, keepdims=True) / width + EPS)
        proj = proj * scale
        head_query = proj[:, :head].astype(BF16)
        head_key = (proj[:, head : 2 * head] * head ** (-0.5)).astype(BF16).astype(F32)
        value = proj[:, 2 * head : 2 * head + rows].astype(BF16).astype(F32)
        outgate = proj[:, 2 * head + rows :].astype(BF16).astype(F32)
        gates = gates * scale
        ingate = gates[:, :heads] + ingate_bias_in[l : l + 1, :]
        logit = gates[:, heads : 2 * heads] + bias
        forget = jnp.minimum(logit, 0.0) - jnp.log1p(jnp.exp(-jnp.abs(logit)))
        shifted = forget + old_stab
        stab = jnp.maximum(shifted, ingate)
        decay = jnp.sum(jnp.where(head_mask, jnp.exp(shifted - stab), 0.0), axis=1, keepdims=True)
        inweight = jnp.sum(
            jnp.where(head_mask, jnp.exp(ingate - stab), 0.0), axis=1, keepdims=True
        )
        gate = head_gain_in[...].astype(F32)[l : l + 1] * jax.nn.sigmoid(outgate)
        query_float = head_query.astype(F32)
        key_dot = jnp.sum(head_key * query_float, axis=1, keepdims=True)
        old = jnp.concatenate((sums[0, l], sums[1, l]), axis=1)
        sum_dot = jnp.sum(old * query_float, axis=1, keepdims=True)
        denominator = jnp.maximum(jnp.abs(decay * sum_dot + inweight * key_dot), 1.0)
        padded = jnp.concatenate((head_query, jnp.zeros((rows - batch, head), BF16)), axis=0)
        factor = gate / denominator
        return padded, decay * factor, inweight * key_dot * value * factor, (
            stab,
            decay,
            inweight,
            head_key,
            value,
        )

    def keep(l, held):
        stab, decay, inweight, head_key, value = held
        keyrow = jnp.where(core == 0, head_key[:, :rows], head_key[:, rows:])
        new_sums[l] = decay * sums[core, l] + inweight * keyrow
        new_stab[l] = stab.T
        vt_ref[...] = jnp.concatenate((value, jnp.zeros((rows - batch, rows), F32)), axis=0).T
        decay_ref[...] = jnp.broadcast_to(decay, (batch, head))
        kk_ref[...] = inweight * head_key

    def readout(l, p, padded, old_factor, fresh):
        off, count = parts[p]
        acc = jnp.zeros((rows, rows), F32)
        for at in range(off, off + count, GROUP):
            c = mem[l, pl.ds(at, GROUP)].reshape(GROUP * rows, head).astype(BF16)
            r = lax.dot_general(
                c, padded, (((1,), (1,)), ((), ())), preferred_element_type=F32
            ).reshape(GROUP, rows, rows)
            for i in range(GROUP):
                acc = jnp.where(lane == at + i, r[i], acc)
        at = slice(off, off + count)
        gath[2 * l + 1, me, pl.ds(off, count)] = (
            old_factor[at] * acc.T[at] + fresh[at]
        ).astype(BF16)

    def update(l, p):
        off, count = parts[p]

        @pl.loop(0, count // GROUP)
        def _(g):
            at = off + g * GROUP
            v = pltpu.roll(vt_ref[...], lax.rem(rows - at, rows), 1)
            for i in range(GROUP):
                mem[l, at + i] = mem[l, at + i] * decay_ref[pl.ds(at + i, 1), :] + v[
                    :, i : i + 1
                ] * kk_ref[pl.ds(at + i, 1), :]

    def output(l, p):
        g = 2 * l + 1
        at = pl.ds(*parts[p])
        moved = None
        for k in range(-1, len(groups)):
            if k < 0:
                arrived(g, p, 3, 1)
            else:
                arrived(g, p, k, 2 * len(groups[k]))
            for c in [chip] if k < 0 else groups[k]:
                x = jnp.concatenate((gath[g, 2 * c, at], gath[g, 2 * c + 1, at]), axis=1)
                w = wout[l, pl.ds(lanes(c * 2 * rows, 2 * rows), 2 * rows), :]
                part = jnp.dot(x, w, preferred_element_type=F32)
                moved = part if moved is None else moved + part
        old = jnp.concatenate((gath[2 * l, 2 * chip, at], gath[2 * l, 2 * chip + 1, at]), axis=1)
        nxt = (old.astype(F32) + moved).astype(BF16)
        gath[g + 1, 2 * chip, at] = nxt[:, :rows]
        if l + 1 < blocks:
            gath[g + 1, 2 * chip + 1, at] = nxt[:, rows:]
            pair_copy(g + 1, p, chip, 3, gsend.at[g + 1], sibling).start()
            for c, group in targets:
                pair_copy(g + 1, p, chip, group, gsend.at[g + 1], c * 2 + 1).start()
        else:
            block_copy(g + 1, p, 2 * chip, 3, gsend.at[g + 1], sibling).start()
            new_tokens[at] = nxt[:, rows:]

    for l in range(blocks):
        loaded(wgi.at[l], local_sem.at[l, 1])
        wgate[l] = wgi[l].astype(F32).reshape(2 * heads, width).astype(BF16)
        if l == 0:
            sums_send.wait()
        ref = wbig.at[l, :, pl.ds(0, 2 * rows)]
        remote(ref, wsend.at[l, 0], wrecv.at[l, 0], sibling).wait()
        padded, old_factor, fresh, held = project(l)
        loaded(mem.at[l], mem_sem.at[l])
        for p in range(len(parts)):
            readout(l, p, padded, old_factor, fresh)
            send_own(2 * l + 1, p)

            @pl.when(core == 0)
            def _():
                block_copy(2 * l + 1, p, me, 3, gsend.at[2 * l + 1], sibling).start()

        keep(l, held)
        if l + 1 < blocks:
            push_weights(l + 1)
        for p in range(len(parts)):
            update(l, p)

        @pl.when(core == 1)
        def _():
            ref = wout.at[l, :, pl.ds(0, rows)]
            remote(ref, wsend.at[l, 1], wrecv.at[l, 1], sibling).wait_recv()
            for p in range(len(parts)):
                output(l, p)

    flushed(gath.at[0, pl.ds(0, chips)], gsend.at[0])

    @pl.when(core == 0)
    def _():
        for l in range(blocks):
            flushed(gath.at[0, pl.ds(0, chips)], gsend.at[2 * l + 1])
            flushed(wout.at[l, :, pl.ds(0, rows)], wsend.at[l, 1])
        for p in range(len(parts)):
            arrived(2 * blocks, p, 3, 1)
            new_tokens[pl.ds(*parts[p])] = gath[2 * blocks, me, pl.ds(*parts[p])]

    @pl.when(core == 1)
    def _():
        for l in range(blocks):
            flushed(gath.at[0, pl.ds(0, chips - 1)], gsend.at[2 * l + 1])
            flushed(gath.at[0, pl.ds(0, n - 2)], gfwd.at[l])
            flushed(gath.at[0, pl.ds(0, n if l + 1 < blocks else 1)], gsend.at[2 * l + 2])


def from_partner(value, axis, stride):
    mask = 2**stride
    pairs = [(source, source ^ mask) for source in range(lax.axis_size(axis))]
    return lax.ppermute(value, axis, pairs)


def plain_body(
    tokens,
    lengths,
    cell_memory,
    key_sums,
    stabilizer,
    norm_gain,
    query_weight,
    key_weight,
    value_weight,
    outgate_weight,
    ingate_weight,
    forget_weight,
    ingate_bias,
    forget_bias,
    forget_slope,
    head_gain,
    output_weight,
):
    devices = lax.axis_size("tp")
    split_count = devices // HEADS
    own_index = lax.axis_index("tp")
    head_id = own_index // split_count
    onehot = (jnp.arange(HEADS) == head_id).astype(jnp.float32)
    position = lengths.astype(jnp.float32) / MAXLEN
    current = tokens
    memories, sums_list, stabs = ([], [], [])
    for block_id in range(cell_memory.shape[0]):
        gathered_rows = lax.all_gather(current, "tp", axis=1, tiled=True)
        row_float = gathered_rows.astype(jnp.float32)
        normed = (
            row_float
            * lax.rsqrt(jnp.mean(row_float * row_float, axis=-1, keepdims=True) + EPS)
            * norm_gain[block_id].astype(jnp.float32)
        ).astype(jnp.bfloat16)
        queries = jnp.dot(
            normed, query_weight[block_id], preferred_element_type=jnp.float32
        ).astype(jnp.bfloat16)
        key_rows = (
            jnp.dot(normed, key_weight[block_id], preferred_element_type=jnp.float32)
            * HEAD ** (-0.5)
        ).astype(jnp.bfloat16)
        values = jnp.dot(normed, value_weight[block_id], preferred_element_type=jnp.float32).astype(
            jnp.bfloat16
        )
        outgate = jnp.dot(
            normed, outgate_weight[block_id], preferred_element_type=jnp.float32
        ).astype(jnp.bfloat16)
        ingate = (
            jnp.dot(normed, ingate_weight[block_id], preferred_element_type=jnp.float32)
            + ingate_bias[block_id]
        )
        forget = jax.nn.log_sigmoid(
            jnp.dot(normed, forget_weight[block_id], preferred_element_type=jnp.float32)
            + forget_bias[block_id]
            + forget_slope[block_id] * position[:, None]
        )
        stab_new = jnp.maximum(forget + stabilizer[block_id], ingate)
        decays = jnp.exp(forget + stabilizer[block_id] - stab_new)
        in_weight = jnp.exp(ingate - stab_new)
        decay_own = jnp.sum(decays * onehot, axis=1)
        inweight_own = jnp.sum(in_weight * onehot, axis=1)
        sums_new = decay_own[:, None] * key_sums[block_id] + inweight_own[
            :, None
        ] * key_rows.astype(jnp.float32)
        head_pair = jnp.stack((queries, key_rows))
        head_sums = sums_new
        for level in range(split_count.bit_length() - 1):
            partner = from_partner(head_pair, "tp", level)
            upper = own_index // (1 << level) % 2 == 1
            lower_half = jnp.where(upper, partner, head_pair)
            upper_half = jnp.where(upper, head_pair, partner)
            head_pair = jnp.concatenate((lower_half, upper_half), axis=2)
            sums_mate = from_partner(head_sums, "tp", level)
            sums_low = jnp.where(upper, sums_mate, head_sums)
            sums_high = jnp.where(upper, head_sums, sums_mate)
            head_sums = jnp.concatenate((sums_low, sums_high), axis=1)
        head_query = head_pair[0].astype(jnp.float32)
        head_keys = head_pair[1].astype(jnp.float32)
        mem_new = (
            decay_own[:, None, None] * cell_memory[block_id]
            + inweight_own[:, None, None]
            * values.astype(jnp.float32)[:, :, None]
            * head_keys[:, None, :]
        )
        numerator = jnp.einsum("bvk,bk->bv", mem_new, head_query, precision=lax.Precision.HIGHEST)
        denominator = jnp.maximum(jnp.abs(jnp.sum(head_sums * head_query, axis=1)), 1.0)
        hidden = numerator / denominator[:, None]
        gated_out = (
            hidden
            * head_gain[block_id].astype(jnp.float32)
            * jax.nn.sigmoid(outgate.astype(jnp.float32))
        ).astype(jnp.bfloat16)
        out_weight = output_weight[block_id]
        projected = jnp.dot(
            lax.all_gather(gated_out, "tp", axis=1, tiled=True),
            out_weight,
            preferred_element_type=jnp.float32,
        )
        current = (current.astype(jnp.float32) + projected).astype(jnp.bfloat16)
        memories.append(mem_new)
        sums_list.append(sums_new)
        stabs.append(stab_new)
    return (current, jnp.stack(memories), jnp.stack(sums_list), jnp.stack(stabs))


def write_out(*refs):
    sems = refs[8]
    copies = [pltpu.make_async_copy(refs[i], refs[4 + i], sems.at[i]) for i in (0, 2, 3)]
    blocks, batch = refs[1].shape[:2]
    for l in range(blocks):
        for g in range(batch // GROUP):
            at = pl.ds(g * GROUP, GROUP)
            copies.append(
                pltpu.make_async_copy(
                    refs[1].at[l, at], refs[5].at[l, at], sems.at[4 + l * (batch // GROUP) + g]
                )
            )
    for c in copies:
        c.start()
    for c in copies:
        c.wait()


def body(*args):
    tokens, lengths, cell_memory, key_sums, stabilizer = args[:5]
    n = lax.axis_size("tp")
    blocks, batch, rows, head = cell_memory.shape
    heads = stabilizer.shape[2]
    width = args[6].shape[1]
    if n != 2 * heads or n % 8 or blocks < 2 or rows < batch or rows % 128 or batch % 16 or batch < 32:
        return plain_body(*args)
    parts = parts_of(batch)
    vm = pl.BlockSpec(memory_space=pltpu.VMEM)
    anyspace = pl.BlockSpec(memory_space=pl.ANY)
    dma = pltpu.SemaphoreType.DMA
    in_specs = [pl.BlockSpec(memory_space=pltpu.HBM)] * 17
    results = pl.pallas_call(
        functools.partial(kernel, n),
        out_shape=(
            pltpu.VMEM((batch, rows), BF16),
            pltpu.VMEM(cell_memory.shape, F32),
            pltpu.VMEM(key_sums.shape, F32),
            pltpu.VMEM((blocks, heads, batch), F32),
        ),
        in_specs=in_specs,
        out_specs=(vm, vm, vm, vm),
        scratch_shapes=[
            pltpu.VMEM((1, batch), jnp.int32),
            pltpu.VMEM((blocks, heads, batch), F32),
            pltpu.VMEM((blocks, width), BF16),
            pltpu.VMEM((blocks, heads), F32),
            pltpu.VMEM((blocks, heads), F32),
            pltpu.VMEM((blocks, heads), F32),
            pltpu.VMEM((blocks, rows), BF16),
            pltpu.VMEM((blocks, width, 2 * head + 2 * rows), BF16),
            pltpu.VMEM((blocks, width, 2 * rows), BF16),
            pltpu.VMEM((blocks, 2, heads, width), BF16),
            pltpu.VMEM((blocks, 2 * heads, width), BF16),
            dma((7,)),
            pltpu.VMEM((2 * blocks + 1, n, batch, rows), BF16),
            pltpu.VMEM((2, blocks, batch, rows), F32),
            pltpu.VMEM((rows, rows), F32),
            pltpu.VMEM((batch, head), F32),
            pltpu.VMEM((batch, head), F32),
            dma((blocks, 4)),
            dma((blocks,)),
            dma((2 * blocks + 1,)),
            dma((blocks,)),
            dma((2 * blocks + 1, len(parts), 4)),
            dma((blocks, 2)),
            dma((blocks, 2)),
            dma,
            dma,
        ],
        compiler_params=pltpu.CompilerParams(
            collective_id=0, has_side_effects=True, vmem_limit_bytes=45500000
        ),
    )(
        tokens,
        lengths.reshape(1, batch),
        cell_memory,
        key_sums,
        stabilizer.swapaxes(1, 2),
        *args[5:10],
        args[10].swapaxes(1, 2),
        args[11].swapaxes(1, 2),
        *args[12:],
    )
    final = pl.pallas_call(
        write_out,
        out_shape=tuple(jax.ShapeDtypeStruct(r.shape, r.dtype) for r in results),
        in_specs=[anyspace] * 4,
        out_specs=(anyspace,) * 4,
        scratch_shapes=[dma((4 + blocks * (batch // GROUP),))],
        compiler_params=pltpu.CompilerParams(vmem_limit_bytes=1024 * 1024),
    )(*results)
    return (*final[:3], final[3].swapaxes(1, 2))


def solution(mesh):
    in_specs = (
        P("grp", "tp"),
        P("grp"),
        P(None, "grp", "tp", None),
        P(None, "grp", "tp"),
        P(None, "grp", None),
        P(),
        P(None, None, "tp"),
        P(None, None, "tp"),
        P(None, None, "tp"),
        P(None, None, "tp"),
        P(),
        P(),
        P(),
        P(),
        P(),
        P(None, "tp"),
        P(None, None, "tp"),
    )
    out_specs = (
        P("grp", "tp"),
        P(None, "grp", "tp", None),
        P(None, "grp", "tp"),
        P(None, "grp", None),
    )
    return jax.shard_map(body, mesh=mesh, in_specs=in_specs, out_specs=out_specs, check_vma=False)
```

```python
import functools

import jax
import jax.numpy as jnp
from jax import lax
from jax.experimental import pallas as pl
from jax.experimental.pallas import tpu as pltpu
from jax.sharding import PartitionSpec as P

HEADS = 8
HEAD = 256
MAXLEN = 4096
EPS = 1e-05
MESH = pl.DeviceIdType.MESH
F32 = jnp.float32
BF16 = jnp.bfloat16
GROUP = 8
FOLD = 16


def parts_of(batch):
    first = 16
    middle = first + (batch - first) // 32 * 16
    return ((0, first), (first, middle - first), (middle, batch - middle))


def kernel(
    n,
    tokens,
    lengths,
    cell_memory,
    key_sums,
    stabilizer,
    norm_gain,
    query_weight,
    key_weight,
    value_weight,
    outgate_weight,
    ingate_weight,
    forget_weight,
    ingate_bias,
    forget_bias,
    forget_slope,
    head_gain,
    output_weight,
    new_tokens,
    mem,
    new_sums,
    new_stab,
    lengths_in,
    stabilizer_in,
    norm_gain_in,
    ingate_bias_in,
    forget_bias_in,
    forget_slope_in,
    head_gain_in,
    wbig,
    wout,
    wgi,
    wgate,
    small_sem,
    gath,
    sums,
    vt_ref,
    decay_ref,
    kk_ref,
    q_ref,
    picks,
    local_sem,
    mem_sem,
    gsend,
    gfwd,
    grecv,
    wsend,
    wrecv,
    ssend,
    srecv,
):
    blocks, batch, rows, head = mem.shape
    heads = stabilizer.shape[1]
    width = output_weight.shape[1]
    split = n // heads
    chips = n // 2
    me = lax.axis_index("tp")
    chip = me // 2
    core = lax.rem(me, 2)
    sibling = me + 1 - 2 * core
    own_head = me // split
    lanes = pl.multiple_of
    parts = parts_of(batch)

    half, quarter = chips // 2, chips // 4
    flip = chip // half
    seat = chip + flip * (chips - 1 - 2 * chip)

    def unflip(d):
        return d + flip * (chips - 1 - 2 * d)

    far_chips = [unflip(chips - 1 - i) for i in range(half)]
    near_chips = [unflip(lax.rem(seat + i, half)) for i in range(1, half)]
    far_group = 2 - seat // quarter
    targets = [(c, far_group) for c in far_chips] + [(c, 0) for c in near_chips]
    groups = (
        near_chips,
        [unflip(half + i) for i in range(quarter)],
        [unflip(half + quarter + i) for i in range(quarter)],
    )

    own_copy = pltpu.make_async_copy(tokens, gath.at[0, me], local_sem.at[0, 3])
    own_copy.start()
    sums_copy = pltpu.make_async_copy(key_sums, sums.at[core], local_sem.at[1, 3])
    small = [
        pltpu.make_async_copy(a, b, small_sem.at[i])
        for i, (a, b) in enumerate(
            (
                (lengths, lengths_in),
                (stabilizer, stabilizer_in),
                (norm_gain, norm_gain_in),
                (ingate_bias, ingate_bias_in),
                (forget_bias, forget_bias_in),
                (forget_slope, forget_slope_in),
                (head_gain, head_gain_in),
            )
        )
    ]
    own_query = pl.ds(lanes(core * rows, rows), rows)
    own_key = pl.ds(lanes(head + core * rows, rows), rows)
    places = (own_query, own_key, pl.ds(2 * head, rows), pl.ds(2 * head + rows, rows))

    def load(l):
        for i, w in enumerate((query_weight, key_weight, value_weight, outgate_weight)):
            pltpu.make_async_copy(w.at[l], wbig.at[l, :, places[i]], local_sem.at[l, 0]).start()
        pltpu.make_async_copy(ingate_weight.at[l], wgi.at[l, 0], local_sem.at[l, 1]).start()
        pltpu.make_async_copy(forget_weight.at[l], wgi.at[l, 1], local_sem.at[l, 1]).start()
        if l == 0:
            for c in small:
                c.start()
            sums_copy.start()
        own = wout.at[l, :, pl.ds(lanes(core * rows, rows), rows)]
        pltpu.make_async_copy(output_weight.at[l], own, local_sem.at[l, 2]).start()
        pltpu.make_async_copy(cell_memory.at[l], mem.at[l], mem_sem.at[l]).start()

    def loaded(ref, sem):
        pltpu.make_async_copy(ref, ref, sem).wait()

    load(0)

    barrier = pltpu.get_barrier_semaphore()
    pl.semaphore_signal(barrier, inc=1, device_id={"tp": sibling}, device_id_type=MESH)

    @pl.when(core == 1)
    def _():
        for c, _ in targets:
            for other in range(2):
                pl.semaphore_signal(
                    barrier, inc=1, device_id={"tp": c * 2 + other}, device_id_type=MESH
                )

    pl.semaphore_wait(barrier, chips)

    def remote(ref, send, recv, dest):
        return pltpu.make_async_remote_copy(
            src_ref=ref,
            dst_ref=ref,
            send_sem=send,
            recv_sem=recv,
            device_id={"tp": dest},
            device_id_type=MESH,
        )

    def block_copy(g, p, slot, group, send, dest):
        return remote(gath.at[g, slot, pl.ds(*parts[p])], send, grecv.at[g, p, group], dest)

    def pair_copy(g, p, c, group, send, dest):
        ref = gath.at[g, pl.ds(2 * c, 2), pl.ds(*parts[p])]
        return remote(ref, send, grecv.at[g, p, group], dest)

    def arrived(g, p, group, count):
        ref = gath.at[g, pl.ds(0, count), pl.ds(*parts[p])]
        remote(ref, gsend.at[g], grecv.at[g, p, group], sibling).wait_recv()

    def flushed(ref, sem):
        remote(ref, sem, wrecv.at[0, 0], sibling).wait_send()

    def send_own(g, p):
        for c, group in targets:
            block_copy(g, p, me, group, gsend.at[g], c * 2 + 1).start()

    def gathered(l, k):
        g = 2 * l
        if k < 0:
            for p in range(len(parts)):
                if l == 0:
                    arrived(g, p, 3, 1)
                else:

                    @pl.when(core == 0)
                    def _():
                        arrived(g, p, 3, 2)

            return [chip]
        for p in range(len(parts)):
            arrived(g, p, k, 2 * len(groups[k]))

            @pl.when(core == 1)
            def _():
                for c in groups[k]:
                    pair_copy(g, p, c, k, gfwd.at[l], sibling).start()

        return groups[k]

    own_copy.wait()
    for p in range(len(parts)):
        block_copy(0, p, me, 3, gsend.at[0], sibling).start()
        send_own(0, p)
    sums_copy.wait()
    sums_send = remote(sums.at[core], ssend, srecv, sibling)
    sums_send.start()

    def push_weights(l):
        loaded(wbig.at[l, :, pl.ds(0, 4 * rows)], local_sem.at[l, 0])
        for place in (own_query, own_key):
            remote(wbig.at[l, :, place], wsend.at[l, 0], wrecv.at[l, 0], sibling).start()
        loaded(wout.at[l, :, pl.ds(0, rows)], local_sem.at[l, 2])

        @pl.when(core == 0)
        def _():
            ref = wout.at[l, :, pl.ds(0, rows)]
            remote(ref, wsend.at[l, 1], wrecv.at[l, 1], sibling).start()

    push_weights(0)
    for l in range(1, blocks):
        load(l)
    for c in small:
        c.wait()
    eye = lax.broadcasted_iota(jnp.int32, (batch, batch), 0) == lax.broadcasted_iota(
        jnp.int32, (batch, batch), 1
    )
    position = jnp.sum(
        jnp.where(eye, lengths_in[...].astype(F32) / MAXLEN, 0.0), axis=1, keepdims=True
    )
    lane = lax.broadcasted_iota(jnp.int32, (rows, rows), 1)

    @pl.loop(0, batch)
    def _(b):
        at = pl.ds(lanes(b * rows, rows), rows)
        picks[at] = jnp.where(lane == b, 1.0, 0.0).astype(BF16)

    head_mask = lax.broadcasted_iota(jnp.int32, (batch, heads), 1) == own_head

    def project(l):
        old_stab = stabilizer_in[l].T
        bias = forget_bias_in[l : l + 1, :] + forget_slope_in[l : l + 1, :] * position

        def step(c, total):
            at = pl.ds(lanes(c * 2 * rows, 2 * rows), 2 * rows)
            x = jnp.concatenate((gath[2 * l, 2 * c], gath[2 * l, 2 * c + 1]), axis=1).astype(F32)
            gain = norm_gain_in[:, at].astype(F32)[l : l + 1]
            scaled = (x * gain).astype(BF16)
            part = jnp.dot(scaled, wbig[l, at, :], preferred_element_type=F32)
            gpart = lax.dot_general(
                scaled, wgate[l, :, at], (((1,), (1,)), ((), ())), preferred_element_type=F32
            )
            square = x * x
            if total is None:
                return part, gpart, square
            return total[0] + part, total[1] + gpart, total[2] + square

        total = None
        for k in range(-1, len(groups)):
            for c in gathered(l, k):
                total = step(c, total)
        proj, gates, square = total
        scale = lax.rsqrt(jnp.sum(square, axis=1, keepdims=True) / width + EPS)
        proj = proj * scale
        head_query = proj[:, :head].astype(BF16)
        head_key = (proj[:, head : 2 * head] * head ** (-0.5)).astype(BF16).astype(F32)
        value = proj[:, 2 * head : 2 * head + rows].astype(BF16).astype(F32)
        outgate = proj[:, 2 * head + rows :].astype(BF16).astype(F32)
        gates = gates * scale
        ingate = gates[:, :heads] + ingate_bias_in[l : l + 1, :]
        logit = gates[:, heads : 2 * heads] + bias
        forget = jnp.minimum(logit, 0.0) - jnp.log1p(jnp.exp(-jnp.abs(logit)))
        shifted = forget + old_stab
        stab = jnp.maximum(shifted, ingate)
        decay = jnp.sum(jnp.where(head_mask, jnp.exp(shifted - stab), 0.0), axis=1, keepdims=True)
        inweight = jnp.sum(
            jnp.where(head_mask, jnp.exp(ingate - stab), 0.0), axis=1, keepdims=True
        )
        gate = head_gain_in[...].astype(F32)[l : l + 1] * jax.nn.sigmoid(outgate)
        query_float = head_query.astype(F32)
        key_dot = jnp.sum(head_key * query_float, axis=1, keepdims=True)
        old = jnp.concatenate((sums[0, l], sums[1, l]), axis=1)
        sum_dot = jnp.sum(old * query_float, axis=1, keepdims=True)
        denominator = jnp.maximum(jnp.abs(decay * sum_dot + inweight * key_dot), 1.0)
        factor = gate / denominator
        q_ref[...] = query_float
        return decay * factor, inweight * key_dot * value * factor, (
            stab,
            decay,
            inweight,
            head_key,
            value,
        )

    def keep(l, held):
        stab, decay, inweight, head_key, value = held
        keyrow = jnp.where(core == 0, head_key[:, :rows], head_key[:, rows:])
        new_sums[l] = decay * sums[core, l] + inweight * keyrow
        new_stab[l] = stab.T
        vt_ref[...] = jnp.concatenate((value, jnp.zeros((rows - batch, rows), F32)), axis=0).T
        decay_ref[...] = jnp.broadcast_to(decay, (batch, head))
        kk_ref[...] = inweight * head_key

    def readout(l, p, old_factor, fresh):
        off, count = parts[p]
        acc = jnp.zeros((rows, rows), F32)
        for at in range(off, off + count, FOLD):
            folded = []
            for b in range(at, at + FOLD):
                product = mem[l, b] * q_ref[pl.ds(b, 1), :]
                folded.append((product[:, :rows] + product[:, rows:]).astype(BF16))
            acc = acc + jnp.dot(
                jnp.concatenate(folded, axis=1),
                picks[pl.ds(at * rows, FOLD * rows), :],
                preferred_element_type=F32,
            )
        at = slice(off, off + count)
        gath[2 * l + 1, me, pl.ds(off, count)] = (
            old_factor[at] * acc.T[at] + fresh[at]
        ).astype(BF16)

    def update(l, p):
        off, count = parts[p]

        @pl.loop(0, count // GROUP)
        def _(g):
            at = off + g * GROUP
            v = pltpu.roll(vt_ref[...], lax.rem(rows - at, rows), 1)
            for i in range(GROUP):
                mem[l, at + i] = mem[l, at + i] * decay_ref[pl.ds(at + i, 1), :] + v[
                    :, i : i + 1
                ] * kk_ref[pl.ds(at + i, 1), :]

    def output(l, p):
        g = 2 * l + 1
        at = pl.ds(*parts[p])
        moved = None
        for k in range(-1, len(groups)):
            if k < 0:
                arrived(g, p, 3, 1)
            else:
                arrived(g, p, k, 2 * len(groups[k]))
            for c in [chip] if k < 0 else groups[k]:
                x = jnp.concatenate((gath[g, 2 * c, at], gath[g, 2 * c + 1, at]), axis=1)
                w = wout[l, pl.ds(lanes(c * 2 * rows, 2 * rows), 2 * rows), :]
                part = jnp.dot(x, w, preferred_element_type=F32)
                moved = part if moved is None else moved + part
        old = jnp.concatenate((gath[2 * l, 2 * chip, at], gath[2 * l, 2 * chip + 1, at]), axis=1)
        nxt = (old.astype(F32) + moved).astype(BF16)
        gath[g + 1, 2 * chip, at] = nxt[:, :rows]
        if l + 1 < blocks:
            gath[g + 1, 2 * chip + 1, at] = nxt[:, rows:]
            pair_copy(g + 1, p, chip, 3, gsend.at[g + 1], sibling).start()
            for c, group in targets:
                pair_copy(g + 1, p, chip, group, gsend.at[g + 1], c * 2 + 1).start()
        else:
            block_copy(g + 1, p, 2 * chip, 3, gsend.at[g + 1], sibling).start()
            new_tokens[at] = nxt[:, rows:]

    for l in range(blocks):
        loaded(wgi.at[l], local_sem.at[l, 1])
        wgate[l] = wgi[l].astype(F32).reshape(2 * heads, width).astype(BF16)
        if l == 0:
            sums_send.wait()
        ref = wbig.at[l, :, pl.ds(0, 2 * rows)]
        remote(ref, wsend.at[l, 0], wrecv.at[l, 0], sibling).wait()
        loaded(mem.at[l], mem_sem.at[l])
        old_factor, fresh, held = project(l)
        for p in range(len(parts)):
            readout(l, p, old_factor, fresh)
            send_own(2 * l + 1, p)

            @pl.when(core == 0)
            def _():
                block_copy(2 * l + 1, p, me, 3, gsend.at[2 * l + 1], sibling).start()

        keep(l, held)
        if l + 1 < blocks:
            push_weights(l + 1)
        for p in range(len(parts)):
            update(l, p)

        @pl.when(core == 1)
        def _():
            ref = wout.at[l, :, pl.ds(0, rows)]
            remote(ref, wsend.at[l, 1], wrecv.at[l, 1], sibling).wait_recv()
            for p in range(len(parts)):
                output(l, p)

    flushed(gath.at[0, pl.ds(0, chips)], gsend.at[0])

    @pl.when(core == 0)
    def _():
        for l in range(blocks):
            flushed(gath.at[0, pl.ds(0, chips)], gsend.at[2 * l + 1])
            flushed(wout.at[l, :, pl.ds(0, rows)], wsend.at[l, 1])
        for p in range(len(parts)):
            arrived(2 * blocks, p, 3, 1)
            new_tokens[pl.ds(*parts[p])] = gath[2 * blocks, me, pl.ds(*parts[p])]

    @pl.when(core == 1)
    def _():
        for l in range(blocks):
            flushed(gath.at[0, pl.ds(0, chips - 1)], gsend.at[2 * l + 1])
            flushed(gath.at[0, pl.ds(0, n - 2)], gfwd.at[l])
            flushed(gath.at[0, pl.ds(0, n if l + 1 < blocks else 1)], gsend.at[2 * l + 2])


def from_partner(value, axis, stride):
    mask = 2**stride
    pairs = [(source, source ^ mask) for source in range(lax.axis_size(axis))]
    return lax.ppermute(value, axis, pairs)


def plain_body(
    tokens,
    lengths,
    cell_memory,
    key_sums,
    stabilizer,
    norm_gain,
    query_weight,
    key_weight,
    value_weight,
    outgate_weight,
    ingate_weight,
    forget_weight,
    ingate_bias,
    forget_bias,
    forget_slope,
    head_gain,
    output_weight,
):
    devices = lax.axis_size("tp")
    split_count = devices // HEADS
    own_index = lax.axis_index("tp")
    head_id = own_index // split_count
    onehot = (jnp.arange(HEADS) == head_id).astype(jnp.float32)
    position = lengths.astype(jnp.float32) / MAXLEN
    current = tokens
    memories, sums_list, stabs = ([], [], [])
    for block_id in range(cell_memory.shape[0]):
        gathered_rows = lax.all_gather(current, "tp", axis=1, tiled=True)
        row_float = gathered_rows.astype(jnp.float32)
        normed = (
            row_float
            * lax.rsqrt(jnp.mean(row_float * row_float, axis=-1, keepdims=True) + EPS)
            * norm_gain[block_id].astype(jnp.float32)
        ).astype(jnp.bfloat16)
        queries = jnp.dot(
            normed, query_weight[block_id], preferred_element_type=jnp.float32
        ).astype(jnp.bfloat16)
        key_rows = (
            jnp.dot(normed, key_weight[block_id], preferred_element_type=jnp.float32)
            * HEAD ** (-0.5)
        ).astype(jnp.bfloat16)
        values = jnp.dot(normed, value_weight[block_id], preferred_element_type=jnp.float32).astype(
            jnp.bfloat16
        )
        outgate = jnp.dot(
            normed, outgate_weight[block_id], preferred_element_type=jnp.float32
        ).astype(jnp.bfloat16)
        ingate = (
            jnp.dot(normed, ingate_weight[block_id], preferred_element_type=jnp.float32)
            + ingate_bias[block_id]
        )
        forget = jax.nn.log_sigmoid(
            jnp.dot(normed, forget_weight[block_id], preferred_element_type=jnp.float32)
            + forget_bias[block_id]
            + forget_slope[block_id] * position[:, None]
        )
        stab_new = jnp.maximum(forget + stabilizer[block_id], ingate)
        decays = jnp.exp(forget + stabilizer[block_id] - stab_new)
        in_weight = jnp.exp(ingate - stab_new)
        decay_own = jnp.sum(decays * onehot, axis=1)
        inweight_own = jnp.sum(in_weight * onehot, axis=1)
        sums_new = decay_own[:, None] * key_sums[block_id] + inweight_own[
            :, None
        ] * key_rows.astype(jnp.float32)
        head_pair = jnp.stack((queries, key_rows))
        head_sums = sums_new
        for level in range(split_count.bit_length() - 1):
            partner = from_partner(head_pair, "tp", level)
            upper = own_index // (1 << level) % 2 == 1
            lower_half = jnp.where(upper, partner, head_pair)
            upper_half = jnp.where(upper, head_pair, partner)
            head_pair = jnp.concatenate((lower_half, upper_half), axis=2)
            sums_mate = from_partner(head_sums, "tp", level)
            sums_low = jnp.where(upper, sums_mate, head_sums)
            sums_high = jnp.where(upper, head_sums, sums_mate)
            head_sums = jnp.concatenate((sums_low, sums_high), axis=1)
        head_query = head_pair[0].astype(jnp.float32)
        head_keys = head_pair[1].astype(jnp.float32)
        mem_new = (
            decay_own[:, None, None] * cell_memory[block_id]
            + inweight_own[:, None, None]
            * values.astype(jnp.float32)[:, :, None]
            * head_keys[:, None, :]
        )
        numerator = jnp.einsum("bvk,bk->bv", mem_new, head_query, precision=lax.Precision.HIGHEST)
        denominator = jnp.maximum(jnp.abs(jnp.sum(head_sums * head_query, axis=1)), 1.0)
        hidden = numerator / denominator[:, None]
        gated_out = (
            hidden
            * head_gain[block_id].astype(jnp.float32)
            * jax.nn.sigmoid(outgate.astype(jnp.float32))
        ).astype(jnp.bfloat16)
        out_weight = output_weight[block_id]
        projected = jnp.dot(
            lax.all_gather(gated_out, "tp", axis=1, tiled=True),
            out_weight,
            preferred_element_type=jnp.float32,
        )
        current = (current.astype(jnp.float32) + projected).astype(jnp.bfloat16)
        memories.append(mem_new)
        sums_list.append(sums_new)
        stabs.append(stab_new)
    return (current, jnp.stack(memories), jnp.stack(sums_list), jnp.stack(stabs))


def write_out(*refs):
    sems = refs[8]
    copies = [pltpu.make_async_copy(refs[i], refs[4 + i], sems.at[i]) for i in (0, 2, 3)]
    blocks, batch = refs[1].shape[:2]
    for l in range(blocks):
        for g in range(batch // GROUP):
            at = pl.ds(g * GROUP, GROUP)
            copies.append(
                pltpu.make_async_copy(
                    refs[1].at[l, at], refs[5].at[l, at], sems.at[4 + l * (batch // GROUP) + g]
                )
            )
    for c in copies:
        c.start()
    for c in copies:
        c.wait()


def body(*args):
    tokens, lengths, cell_memory, key_sums, stabilizer = args[:5]
    n = lax.axis_size("tp")
    blocks, batch, rows, head = cell_memory.shape
    heads = stabilizer.shape[2]
    width = args[6].shape[1]
    if n != 2 * heads or n % 8 or blocks < 2 or rows < batch or rows % 128 or batch % 16 or batch < 48:
        return plain_body(*args)
    parts = parts_of(batch)
    vm = pl.BlockSpec(memory_space=pltpu.VMEM)
    anyspace = pl.BlockSpec(memory_space=pl.ANY)
    dma = pltpu.SemaphoreType.DMA
    in_specs = [pl.BlockSpec(memory_space=pltpu.HBM)] * 17
    results = pl.pallas_call(
        functools.partial(kernel, n),
        out_shape=(
            pltpu.VMEM((batch, rows), BF16),
            pltpu.VMEM(cell_memory.shape, F32),
            pltpu.VMEM(key_sums.shape, F32),
            pltpu.VMEM((blocks, heads, batch), F32),
        ),
        in_specs=in_specs,
        out_specs=(vm, vm, vm, vm),
        scratch_shapes=[
            pltpu.VMEM((1, batch), jnp.int32),
            pltpu.VMEM((blocks, heads, batch), F32),
            pltpu.VMEM((blocks, width), BF16),
            pltpu.VMEM((blocks, heads), F32),
            pltpu.VMEM((blocks, heads), F32),
            pltpu.VMEM((blocks, heads), F32),
            pltpu.VMEM((blocks, rows), BF16),
            pltpu.VMEM((blocks, width, 2 * head + 2 * rows), BF16),
            pltpu.VMEM((blocks, width, 2 * rows), BF16),
            pltpu.VMEM((blocks, 2, heads, width), BF16),
            pltpu.VMEM((blocks, 2 * heads, width), BF16),
            dma((7,)),
            pltpu.VMEM((2 * blocks + 1, n, batch, rows), BF16),
            pltpu.VMEM((2, blocks, batch, rows), F32),
            pltpu.VMEM((rows, rows), F32),
            pltpu.VMEM((batch, head), F32),
            pltpu.VMEM((batch, head), F32),
            pltpu.VMEM((batch, head), F32),
            pltpu.VMEM((batch * rows, rows), BF16),
            dma((blocks, 4)),
            dma((blocks,)),
            dma((2 * blocks + 1,)),
            dma((blocks,)),
            dma((2 * blocks + 1, len(parts), 4)),
            dma((blocks, 2)),
            dma((blocks, 2)),
            dma,
            dma,
        ],
        compiler_params=pltpu.CompilerParams(
            collective_id=0, has_side_effects=True, vmem_limit_bytes=45500000
        ),
    )(
        tokens,
        lengths.reshape(1, batch),
        cell_memory,
        key_sums,
        stabilizer.swapaxes(1, 2),
        *args[5:10],
        args[10].swapaxes(1, 2),
        args[11].swapaxes(1, 2),
        *args[12:],
    )
    final = pl.pallas_call(
        write_out,
        out_shape=tuple(jax.ShapeDtypeStruct(r.shape, r.dtype) for r in results),
        in_specs=[anyspace] * 4,
        out_specs=(anyspace,) * 4,
        scratch_shapes=[dma((4 + blocks * (batch // GROUP),))],
        compiler_params=pltpu.CompilerParams(vmem_limit_bytes=1024 * 1024),
    )(*results)
    return (*final[:3], final[3].swapaxes(1, 2))


def solution(mesh):
    in_specs = (
        P("grp", "tp"),
        P("grp"),
        P(None, "grp", "tp", None),
        P(None, "grp", "tp"),
        P(None, "grp", None),
        P(),
        P(None, None, "tp"),
        P(None, None, "tp"),
        P(None, None, "tp"),
        P(None, None, "tp"),
        P(),
        P(),
        P(),
        P(),
        P(),
        P(None, "tp"),
        P(None, None, "tp"),
    )
    out_specs = (
        P("grp", "tp"),
        P(None, "grp", "tp", None),
        P(None, "grp", "tp"),
        P(None, "grp", None),
    )
    return jax.shard_map(body, mesh=mesh, in_specs=in_specs, out_specs=out_specs, check_vma=False)
```

```python
import functools

import jax
import jax.numpy as jnp
from jax import lax
from jax.experimental import pallas as pl
from jax.experimental.pallas import tpu as pltpu
from jax.sharding import PartitionSpec as P

HEADS = 8
HEAD = 256
MAXLEN = 4096
EPS = 1e-05
MESH = pl.DeviceIdType.MESH
F32 = jnp.float32
BF16 = jnp.bfloat16
GROUP = 8
FOLD = 16


def parts_of(batch):
    return ((0, 16), (16, 16), (32, batch - 32))


def kernel(
    n,
    tokens,
    lengths,
    cell_memory,
    key_sums,
    stabilizer,
    norm_gain,
    query_weight,
    key_weight,
    value_weight,
    outgate_weight,
    ingate_weight,
    forget_weight,
    ingate_bias,
    forget_bias,
    forget_slope,
    head_gain,
    output_weight,
    new_tokens,
    mem,
    new_sums,
    new_stab,
    lengths_in,
    stabilizer_in,
    norm_gain_in,
    ingate_bias_in,
    forget_bias_in,
    forget_slope_in,
    head_gain_in,
    wbig,
    wout,
    wgi,
    wgate,
    small_sem,
    gath,
    sums,
    vt_ref,
    decay_ref,
    kk_ref,
    q_ref,
    picks,
    local_sem,
    mem_sem,
    gsend,
    gfwd,
    grecv,
    wsend,
    wrecv,
    ssend,
    srecv,
):
    blocks, batch, rows, head = mem.shape
    heads = stabilizer.shape[1]
    width = output_weight.shape[1]
    split = n // heads
    chips = n // 2
    me = lax.axis_index("tp")
    chip = me // 2
    core = lax.rem(me, 2)
    sibling = me + 1 - 2 * core
    own_head = me // split
    lanes = pl.multiple_of
    parts = parts_of(batch)

    half, quarter = chips // 2, chips // 4
    flip = chip // half
    seat = chip + flip * (chips - 1 - 2 * chip)

    def unflip(d):
        return d + flip * (chips - 1 - 2 * d)

    far_chips = [unflip(chips - 1 - i) for i in range(half)]
    near_chips = [unflip(lax.rem(seat + i, half)) for i in range(1, half)]
    far_group = 2 - seat // quarter
    targets = [(c, far_group) for c in far_chips] + [(c, 0) for c in near_chips]
    groups = (
        near_chips,
        [unflip(half + i) for i in range(quarter)],
        [unflip(half + quarter + i) for i in range(quarter)],
    )

    own_copy = pltpu.make_async_copy(tokens, gath.at[0, me], local_sem.at[0, 3])
    own_copy.start()
    sums_copy = pltpu.make_async_copy(key_sums, sums.at[core], local_sem.at[1, 3])
    small = [
        pltpu.make_async_copy(a, b, small_sem.at[i])
        for i, (a, b) in enumerate(
            (
                (lengths, lengths_in),
                (stabilizer, stabilizer_in),
                (norm_gain, norm_gain_in),
                (ingate_bias, ingate_bias_in),
                (forget_bias, forget_bias_in),
                (forget_slope, forget_slope_in),
                (head_gain, head_gain_in),
            )
        )
    ]
    own_query = pl.ds(lanes(core * rows, rows), rows)
    own_key = pl.ds(lanes(head + core * rows, rows), rows)
    places = (own_query, own_key, pl.ds(2 * head, rows), pl.ds(2 * head + rows, rows))

    def load(l):
        for i, w in enumerate((query_weight, key_weight, value_weight, outgate_weight)):
            pltpu.make_async_copy(w.at[l], wbig.at[l, :, places[i]], local_sem.at[l, 0]).start()
        pltpu.make_async_copy(ingate_weight.at[l], wgi.at[l, 0], local_sem.at[l, 1]).start()
        pltpu.make_async_copy(forget_weight.at[l], wgi.at[l, 1], local_sem.at[l, 1]).start()
        if l == 0:
            for c in small:
                c.start()
            sums_copy.start()
        own = wout.at[l, :, pl.ds(lanes(core * rows, rows), rows)]
        pltpu.make_async_copy(output_weight.at[l], own, local_sem.at[l, 2]).start()
        pltpu.make_async_copy(cell_memory.at[l], mem.at[l], mem_sem.at[l]).start()

    def loaded(ref, sem):
        pltpu.make_async_copy(ref, ref, sem).wait()

    load(0)

    barrier = pltpu.get_barrier_semaphore()
    pl.semaphore_signal(barrier, inc=1, device_id={"tp": sibling}, device_id_type=MESH)

    @pl.when(core == 1)
    def _():
        for c, _ in targets:
            for other in range(2):
                pl.semaphore_signal(
                    barrier, inc=1, device_id={"tp": c * 2 + other}, device_id_type=MESH
                )

    pl.semaphore_wait(barrier, chips)

    def remote(ref, send, recv, dest):
        return pltpu.make_async_remote_copy(
            src_ref=ref,
            dst_ref=ref,
            send_sem=send,
            recv_sem=recv,
            device_id={"tp": dest},
            device_id_type=MESH,
        )

    last = len(parts) - 1

    def signal(g, p, group):
        if p < last:
            return grecv.at[g, 2 * p + (group == 3)]
        return grecv.at[g, 2 * last + group]

    def block_copy(g, p, slot, group, send, dest):
        return remote(gath.at[g, slot, pl.ds(*parts[p])], send, signal(g, p, group), dest)

    def pair_copy(g, p, c, group, send, dest):
        ref = gath.at[g, pl.ds(2 * c, 2), pl.ds(*parts[p])]
        return remote(ref, send, signal(g, p, group), dest)

    def arrived(g, p, group, count):
        ref = gath.at[g, pl.ds(0, count), pl.ds(*parts[p])]
        remote(ref, gsend.at[g], signal(g, p, group), sibling).wait_recv()

    def flushed(ref, sem):
        remote(ref, sem, wrecv.at[0, 0], sibling).wait_send()

    def send_own(g, p):
        for c, group in targets:
            group = group if p == last else 0
            block_copy(g, p, me, group, gsend.at[g], c * 2 + 1).start()

    def gathered(l, k):
        g = 2 * l
        if k < 0:
            for p in range(len(parts)):
                if l == 0:
                    arrived(g, p, 3, 1)
                else:

                    @pl.when(core == 0)
                    def _():
                        arrived(g, p, 3, 2)

            return [chip]
        for p in range(len(parts)):
            if p < last and k > 0:
                continue
            here = groups[k] if p == last else sum(groups, [])
            arrived(g, p, k, 2 * len(here))

            @pl.when(core == 1)
            def _():
                for c in here:
                    pair_copy(g, p, c, k, gfwd.at[l], sibling).start()

        return groups[k]

    own_copy.wait()
    for p in range(len(parts)):
        block_copy(0, p, me, 3, gsend.at[0], sibling).start()
        send_own(0, p)
    sums_copy.wait()
    sums_send = remote(sums.at[core], ssend, srecv, sibling)
    sums_send.start()

    def push_weights(l):
        loaded(wbig.at[l, :, pl.ds(0, 4 * rows)], local_sem.at[l, 0])
        for place in (own_query, own_key):
            remote(wbig.at[l, :, place], wsend.at[l, 0], wrecv.at[l, 0], sibling).start()
        loaded(wout.at[l, :, pl.ds(0, rows)], local_sem.at[l, 2])

        @pl.when(core == 0)
        def _():
            ref = wout.at[l, :, pl.ds(0, rows)]
            remote(ref, wsend.at[l, 1], wrecv.at[l, 1], sibling).start()

    push_weights(0)
    for l in range(1, blocks):
        load(l)
    for c in small:
        c.wait()
    eye = lax.broadcasted_iota(jnp.int32, (batch, batch), 0) == lax.broadcasted_iota(
        jnp.int32, (batch, batch), 1
    )
    position = jnp.sum(
        jnp.where(eye, lengths_in[...].astype(F32) / MAXLEN, 0.0), axis=1, keepdims=True
    )
    lane = lax.broadcasted_iota(jnp.int32, (rows, rows), 1)

    @pl.loop(0, batch)
    def _(b):
        at = pl.ds(lanes(b * rows, rows), rows)
        picks[at] = jnp.where(lane == b, 1.0, 0.0).astype(BF16)

    head_mask = lax.broadcasted_iota(jnp.int32, (batch, heads), 1) == own_head

    def project(l):
        old_stab = stabilizer_in[l].T
        bias = forget_bias_in[l : l + 1, :] + forget_slope_in[l : l + 1, :] * position

        def step(c, total):
            at = pl.ds(lanes(c * 2 * rows, 2 * rows), 2 * rows)
            x = jnp.concatenate((gath[2 * l, 2 * c], gath[2 * l, 2 * c + 1]), axis=1).astype(F32)
            gain = norm_gain_in[:, at].astype(F32)[l : l + 1]
            scaled = (x * gain).astype(BF16)
            part = jnp.dot(scaled, wbig[l, at, :], preferred_element_type=F32)
            gpart = lax.dot_general(
                scaled, wgate[l, :, at], (((1,), (1,)), ((), ())), preferred_element_type=F32
            )
            square = x * x
            if total is None:
                return part, gpart, square
            return total[0] + part, total[1] + gpart, total[2] + square

        total = None
        for k in range(-1, len(groups)):
            for c in gathered(l, k):
                total = step(c, total)
        proj, gates, square = total
        scale = lax.rsqrt(jnp.sum(square, axis=1, keepdims=True) / width + EPS)
        proj = proj * scale
        head_query = proj[:, :head].astype(BF16)
        head_key = (proj[:, head : 2 * head] * head ** (-0.5)).astype(BF16).astype(F32)
        value = proj[:, 2 * head : 2 * head + rows].astype(BF16).astype(F32)
        outgate = proj[:, 2 * head + rows :].astype(BF16).astype(F32)
        gates = gates * scale
        ingate = gates[:, :heads] + ingate_bias_in[l : l + 1, :]
        logit = gates[:, heads : 2 * heads] + bias
        forget = jnp.minimum(logit, 0.0) - jnp.log1p(jnp.exp(-jnp.abs(logit)))
        shifted = forget + old_stab
        stab = jnp.maximum(shifted, ingate)
        decay = jnp.sum(jnp.where(head_mask, jnp.exp(shifted - stab), 0.0), axis=1, keepdims=True)
        inweight = jnp.sum(
            jnp.where(head_mask, jnp.exp(ingate - stab), 0.0), axis=1, keepdims=True
        )
        gate = head_gain_in[...].astype(F32)[l : l + 1] * jax.nn.sigmoid(outgate)
        query_float = head_query.astype(F32)
        key_dot = jnp.sum(head_key * query_float, axis=1, keepdims=True)
        old = jnp.concatenate((sums[0, l], sums[1, l]), axis=1)
        sum_dot = jnp.sum(old * query_float, axis=1, keepdims=True)
        denominator = jnp.maximum(jnp.abs(decay * sum_dot + inweight * key_dot), 1.0)
        factor = gate / denominator
        q_ref[...] = query_float
        return decay * factor, inweight * key_dot * value * factor, (
            stab,
            decay,
            inweight,
            head_key,
            value,
        )

    def keep(l, held):
        stab, decay, inweight, head_key, value = held
        keyrow = jnp.where(core == 0, head_key[:, :rows], head_key[:, rows:])
        new_sums[l] = decay * sums[core, l] + inweight * keyrow
        new_stab[l] = stab.T
        vt_ref[...] = jnp.concatenate((value, jnp.zeros((rows - batch, rows), F32)), axis=0).T
        decay_ref[...] = jnp.broadcast_to(decay, (batch, head))
        kk_ref[...] = inweight * head_key

    def readout(l, p, old_factor, fresh):
        off, count = parts[p]
        acc = jnp.zeros((rows, rows), F32)
        for at in range(off, off + count, FOLD):
            folded = []
            for b in range(at, at + FOLD):
                product = mem[l, b] * q_ref[pl.ds(b, 1), :]
                folded.append((product[:, :rows] + product[:, rows:]).astype(BF16))
            acc = acc + jnp.dot(
                jnp.concatenate(folded, axis=1),
                picks[pl.ds(at * rows, FOLD * rows), :],
                preferred_element_type=F32,
            )
        at = slice(off, off + count)
        gath[2 * l + 1, me, pl.ds(off, count)] = (
            old_factor[at] * acc.T[at] + fresh[at]
        ).astype(BF16)

    def update(l, p):
        off, count = parts[p]

        @pl.loop(0, count // GROUP)
        def _(g):
            at = off + g * GROUP
            v = pltpu.roll(vt_ref[...], lax.rem(rows - at, rows), 1)
            for i in range(GROUP):
                mem[l, at + i] = mem[l, at + i] * decay_ref[pl.ds(at + i, 1), :] + v[
                    :, i : i + 1
                ] * kk_ref[pl.ds(at + i, 1), :]

    def output(l, p):
        g = 2 * l + 1
        at = pl.ds(*parts[p])
        moved = None
        for k in range(-1, len(groups)):
            if k < 0:
                arrived(g, p, 3, 1)
            elif p == last:
                arrived(g, p, k, 2 * len(groups[k]))
            elif k == 0:
                arrived(g, p, k, n - 2)
            for c in [chip] if k < 0 else groups[k]:
                x = jnp.concatenate((gath[g, 2 * c, at], gath[g, 2 * c + 1, at]), axis=1)
                w = wout[l, pl.ds(lanes(c * 2 * rows, 2 * rows), 2 * rows), :]
                part = jnp.dot(x, w, preferred_element_type=F32)
                moved = part if moved is None else moved + part
        old = jnp.concatenate((gath[2 * l, 2 * chip, at], gath[2 * l, 2 * chip + 1, at]), axis=1)
        nxt = (old.astype(F32) + moved).astype(BF16)
        gath[g + 1, 2 * chip, at] = nxt[:, :rows]
        if l + 1 < blocks:
            gath[g + 1, 2 * chip + 1, at] = nxt[:, rows:]
            pair_copy(g + 1, p, chip, 3, gsend.at[g + 1], sibling).start()
            for c, group in targets:
                group = group if p == last else 0
                pair_copy(g + 1, p, chip, group, gsend.at[g + 1], c * 2 + 1).start()
        else:
            block_copy(g + 1, p, 2 * chip, 3, gsend.at[g + 1], sibling).start()
            new_tokens[at] = nxt[:, rows:]

    for l in range(blocks):
        loaded(wgi.at[l], local_sem.at[l, 1])
        wgate[l] = wgi[l].astype(F32).reshape(2 * heads, width).astype(BF16)
        if l == 0:
            sums_send.wait()
        ref = wbig.at[l, :, pl.ds(0, 2 * rows)]
        remote(ref, wsend.at[l, 0], wrecv.at[l, 0], sibling).wait()
        loaded(mem.at[l], mem_sem.at[l])
        old_factor, fresh, held = project(l)
        for p in range(len(parts)):
            readout(l, p, old_factor, fresh)
            send_own(2 * l + 1, p)

            @pl.when(core == 0)
            def _():
                block_copy(2 * l + 1, p, me, 3, gsend.at[2 * l + 1], sibling).start()

        keep(l, held)
        if l + 1 < blocks:
            push_weights(l + 1)
        for p in range(len(parts)):
            update(l, p)

        @pl.when(core == 1)
        def _():
            ref = wout.at[l, :, pl.ds(0, rows)]
            remote(ref, wsend.at[l, 1], wrecv.at[l, 1], sibling).wait_recv()
            for p in range(len(parts)):
                output(l, p)

    flushed(gath.at[0, pl.ds(0, chips)], gsend.at[0])

    @pl.when(core == 0)
    def _():
        for l in range(blocks):
            flushed(gath.at[0, pl.ds(0, chips)], gsend.at[2 * l + 1])
            flushed(wout.at[l, :, pl.ds(0, rows)], wsend.at[l, 1])
        for p in range(len(parts)):
            arrived(2 * blocks, p, 3, 1)
            new_tokens[pl.ds(*parts[p])] = gath[2 * blocks, me, pl.ds(*parts[p])]

    @pl.when(core == 1)
    def _():
        for l in range(blocks):
            flushed(gath.at[0, pl.ds(0, chips - 1)], gsend.at[2 * l + 1])
            flushed(gath.at[0, pl.ds(0, n - 2)], gfwd.at[l])
            flushed(gath.at[0, pl.ds(0, n if l + 1 < blocks else 1)], gsend.at[2 * l + 2])


def from_partner(value, axis, stride):
    mask = 2**stride
    pairs = [(source, source ^ mask) for source in range(lax.axis_size(axis))]
    return lax.ppermute(value, axis, pairs)


def plain_body(
    tokens,
    lengths,
    cell_memory,
    key_sums,
    stabilizer,
    norm_gain,
    query_weight,
    key_weight,
    value_weight,
    outgate_weight,
    ingate_weight,
    forget_weight,
    ingate_bias,
    forget_bias,
    forget_slope,
    head_gain,
    output_weight,
):
    devices = lax.axis_size("tp")
    split_count = devices // HEADS
    own_index = lax.axis_index("tp")
    head_id = own_index // split_count
    onehot = (jnp.arange(HEADS) == head_id).astype(jnp.float32)
    position = lengths.astype(jnp.float32) / MAXLEN
    current = tokens
    memories, sums_list, stabs = ([], [], [])
    for block_id in range(cell_memory.shape[0]):
        gathered_rows = lax.all_gather(current, "tp", axis=1, tiled=True)
        row_float = gathered_rows.astype(jnp.float32)
        normed = (
            row_float
            * lax.rsqrt(jnp.mean(row_float * row_float, axis=-1, keepdims=True) + EPS)
            * norm_gain[block_id].astype(jnp.float32)
        ).astype(jnp.bfloat16)
        queries = jnp.dot(
            normed, query_weight[block_id], preferred_element_type=jnp.float32
        ).astype(jnp.bfloat16)
        key_rows = (
            jnp.dot(normed, key_weight[block_id], preferred_element_type=jnp.float32)
            * HEAD ** (-0.5)
        ).astype(jnp.bfloat16)
        values = jnp.dot(normed, value_weight[block_id], preferred_element_type=jnp.float32).astype(
            jnp.bfloat16
        )
        outgate = jnp.dot(
            normed, outgate_weight[block_id], preferred_element_type=jnp.float32
        ).astype(jnp.bfloat16)
        ingate = (
            jnp.dot(normed, ingate_weight[block_id], preferred_element_type=jnp.float32)
            + ingate_bias[block_id]
        )
        forget = jax.nn.log_sigmoid(
            jnp.dot(normed, forget_weight[block_id], preferred_element_type=jnp.float32)
            + forget_bias[block_id]
            + forget_slope[block_id] * position[:, None]
        )
        stab_new = jnp.maximum(forget + stabilizer[block_id], ingate)
        decays = jnp.exp(forget + stabilizer[block_id] - stab_new)
        in_weight = jnp.exp(ingate - stab_new)
        decay_own = jnp.sum(decays * onehot, axis=1)
        inweight_own = jnp.sum(in_weight * onehot, axis=1)
        sums_new = decay_own[:, None] * key_sums[block_id] + inweight_own[
            :, None
        ] * key_rows.astype(jnp.float32)
        head_pair = jnp.stack((queries, key_rows))
        head_sums = sums_new
        for level in range(split_count.bit_length() - 1):
            partner = from_partner(head_pair, "tp", level)
            upper = own_index // (1 << level) % 2 == 1
            lower_half = jnp.where(upper, partner, head_pair)
            upper_half = jnp.where(upper, head_pair, partner)
            head_pair = jnp.concatenate((lower_half, upper_half), axis=2)
            sums_mate = from_partner(head_sums, "tp", level)
            sums_low = jnp.where(upper, sums_mate, head_sums)
            sums_high = jnp.where(upper, head_sums, sums_mate)
            head_sums = jnp.concatenate((sums_low, sums_high), axis=1)
        head_query = head_pair[0].astype(jnp.float32)
        head_keys = head_pair[1].astype(jnp.float32)
        mem_new = (
            decay_own[:, None, None] * cell_memory[block_id]
            + inweight_own[:, None, None]
            * values.astype(jnp.float32)[:, :, None]
            * head_keys[:, None, :]
        )
        numerator = jnp.einsum("bvk,bk->bv", mem_new, head_query, precision=lax.Precision.HIGHEST)
        denominator = jnp.maximum(jnp.abs(jnp.sum(head_sums * head_query, axis=1)), 1.0)
        hidden = numerator / denominator[:, None]
        gated_out = (
            hidden
            * head_gain[block_id].astype(jnp.float32)
            * jax.nn.sigmoid(outgate.astype(jnp.float32))
        ).astype(jnp.bfloat16)
        out_weight = output_weight[block_id]
        projected = jnp.dot(
            lax.all_gather(gated_out, "tp", axis=1, tiled=True),
            out_weight,
            preferred_element_type=jnp.float32,
        )
        current = (current.astype(jnp.float32) + projected).astype(jnp.bfloat16)
        memories.append(mem_new)
        sums_list.append(sums_new)
        stabs.append(stab_new)
    return (current, jnp.stack(memories), jnp.stack(sums_list), jnp.stack(stabs))


def write_out(*refs):
    sems = refs[8]
    copies = [pltpu.make_async_copy(refs[i], refs[4 + i], sems.at[i]) for i in (0, 2, 3)]
    blocks, batch = refs[1].shape[:2]
    for l in range(blocks):
        for g in range(batch // GROUP):
            at = pl.ds(g * GROUP, GROUP)
            copies.append(
                pltpu.make_async_copy(
                    refs[1].at[l, at], refs[5].at[l, at], sems.at[4 + l * (batch // GROUP) + g]
                )
            )
    for c in copies:
        c.start()
    for c in copies:
        c.wait()


def body(*args):
    tokens, lengths, cell_memory, key_sums, stabilizer = args[:5]
    n = lax.axis_size("tp")
    blocks, batch, rows, head = cell_memory.shape
    heads = stabilizer.shape[2]
    width = args[6].shape[1]
    if n != 2 * heads or n % 8 or blocks < 2 or rows < batch or rows % 128 or batch % 16 or batch < 48:
        return plain_body(*args)
    parts = parts_of(batch)
    vm = pl.BlockSpec(memory_space=pltpu.VMEM)
    anyspace = pl.BlockSpec(memory_space=pl.ANY)
    dma = pltpu.SemaphoreType.DMA
    in_specs = [pl.BlockSpec(memory_space=pltpu.HBM)] * 17
    results = pl.pallas_call(
        functools.partial(kernel, n),
        out_shape=(
            pltpu.VMEM((batch, rows), BF16),
            pltpu.VMEM(cell_memory.shape, F32),
            pltpu.VMEM(key_sums.shape, F32),
            pltpu.VMEM((blocks, heads, batch), F32),
        ),
        in_specs=in_specs,
        out_specs=(vm, vm, vm, vm),
        scratch_shapes=[
            pltpu.VMEM((1, batch), jnp.int32),
            pltpu.VMEM((blocks, heads, batch), F32),
            pltpu.VMEM((blocks, width), BF16),
            pltpu.VMEM((blocks, heads), F32),
            pltpu.VMEM((blocks, heads), F32),
            pltpu.VMEM((blocks, heads), F32),
            pltpu.VMEM((blocks, rows), BF16),
            pltpu.VMEM((blocks, width, 2 * head + 2 * rows), BF16),
            pltpu.VMEM((blocks, width, 2 * rows), BF16),
            pltpu.VMEM((blocks, 2, heads, width), BF16),
            pltpu.VMEM((blocks, 2 * heads, width), BF16),
            dma((7,)),
            pltpu.VMEM((2 * blocks + 1, n, batch, rows), BF16),
            pltpu.VMEM((2, blocks, batch, rows), F32),
            pltpu.VMEM((rows, rows), F32),
            pltpu.VMEM((batch, head), F32),
            pltpu.VMEM((batch, head), F32),
            pltpu.VMEM((batch, head), F32),
            pltpu.VMEM((batch * rows, rows), BF16),
            dma((blocks, 4)),
            dma((blocks,)),
            dma((2 * blocks + 1,)),
            dma((blocks,)),
            dma((2 * blocks + 1, 2 * len(parts) + 2)),
            dma((blocks, 2)),
            dma((blocks, 2)),
            dma,
            dma,
        ],
        compiler_params=pltpu.CompilerParams(
            collective_id=0, has_side_effects=True, vmem_limit_bytes=45500000
        ),
    )(
        tokens,
        lengths.reshape(1, batch),
        cell_memory,
        key_sums,
        stabilizer.swapaxes(1, 2),
        *args[5:10],
        args[10].swapaxes(1, 2),
        args[11].swapaxes(1, 2),
        *args[12:],
    )
    final = pl.pallas_call(
        write_out,
        out_shape=tuple(jax.ShapeDtypeStruct(r.shape, r.dtype) for r in results),
        in_specs=[anyspace] * 4,
        out_specs=(anyspace,) * 4,
        scratch_shapes=[dma((4 + blocks * (batch // GROUP),))],
        compiler_params=pltpu.CompilerParams(vmem_limit_bytes=1024 * 1024),
    )(*results)
    return (*final[:3], final[3].swapaxes(1, 2))


def solution(mesh):
    in_specs = (
        P("grp", "tp"),
        P("grp"),
        P(None, "grp", "tp", None),
        P(None, "grp", "tp"),
        P(None, "grp", None),
        P(),
        P(None, None, "tp"),
        P(None, None, "tp"),
        P(None, None, "tp"),
        P(None, None, "tp"),
        P(),
        P(),
        P(),
        P(),
        P(),
        P(None, "tp"),
        P(None, None, "tp"),
    )
    out_specs = (
        P("grp", "tp"),
        P(None, "grp", "tp", None),
        P(None, "grp", "tp"),
        P(None, "grp", None),
    )
    return jax.shard_map(body, mesh=mesh, in_specs=in_specs, out_specs=out_specs, check_vma=False)
```
